256 devices in a mesh: sp: 64 (over z, x, core), tp: 4 (over y).
Axes of the slice: x: 4, y: 4, z: 8, core: 2. Of those that a mesh axis runs over, the one named last changes fastest.
Arguments:
- residual: bfloat16 [16384, 2048], P(('sp', 'tp')), may hold values from -6 to 6
- query_vectors: bfloat16 [16384, 512], P('sp', 'tp'), may hold values from -6 to 6
- key_vectors: bfloat16 [16384, 512], P('sp', 'tp'), may hold values from -6 to 6
- value_vectors: bfloat16 [16384, 512], P('sp', 'tp'), may hold values from -6 to 6
- in_gate: float32 [8, 16384], P('tp', 'sp'), may hold values from -9 to 190
- forget_gate: float32 [8, 16384], P('tp', 'sp'), may hold values from -1 to 12
- documents: int32 [16384], P('sp'), may hold values from 0 to 15, never falling along the last dimension, each value on 1 to 2048 neighbouring positions
- w_out: bfloat16 [512, 2048], P('tp'), may hold values from -0.25 to 0.25
- norm_gain: bfloat16 [2048], replicated, may hold values from 0.099609375 to 1.8984375
- w_up: bfloat16 [2048, 8192], P('sp', 'tp'), may hold values from -0.125 to 0.125
- w_down: bfloat16 [8192, 2048], P('tp', 'sp'), may hold values from -0.0625 to 0.0625
Outputs:
- layer_out: bfloat16 [16384, 2048], P(('sp', 'tp'))
The draws below stay inside these ranges and needn't reach their ends.
Inputs may be any that keep to these rules, and one draw needn't show every extreme that they name: `documents`: document numbers never fall along the positions; every document has 1 to 2048 positions.
All inputs are finite; a program needn't handle non-finite values.
Results may differ from the reference program's by a relative error of at most 0.015.
Values may be sent and summed in bfloat16 or wider, within the bound.
No kernel may reach another device: no remote copies, remote signals or barrier semaphores. Data moves between devices by JAX's collectives and lax.ppermute only.
A program may use at most 64 MiB of HBM per device.

```python
import math
import jax
import jax.numpy as jnp
import numpy as np
from jax import lax

D = 2048
MEMORY_HEADS = 8
FF = 8192
SPAN = 128
TOK_DEV = 256
HW = 512
PACKED_TOKENS = 16384
DOCS = 16
DOC_MOST = 2048
N_TP = 4


def draw_in_gate(key, part):
    base_key = jax.random.fold_in(key, 0)
    drawn = jnp.clip(jax.random.normal(base_key, (MEMORY_HEADS, PACKED_TOKENS), jnp.float32), -5.5, 4.5) - 3.5
    return drawn


def draw_forget_gate(key, part):
    shuffle_random_key, gradual_random_key, quick_random_key, block_random_key, jitter_random_key, spike_random_key, dropout_random_key = jax.random.split(key, 7)
    head_order = jax.random.permutation(shuffle_random_key, MEMORY_HEADS)
    slow_count = MEMORY_HEADS // 2
    slow_heads = head_order < slow_count
    slow_rate = math.log(10.0) / DOC_MOST * jax.random.uniform(gradual_random_key, (MEMORY_HEADS,), jnp.float32, 0.3, 1.0)
    fast_rate = 1.0 / jax.random.uniform(quick_random_key, (MEMORY_HEADS,), jnp.float32, 30.0, 100.0)
    head_rate = jnp.where(slow_heads, slow_rate, fast_rate)
    block_factor = jnp.exp(jax.random.uniform(block_random_key, (PACKED_TOKENS // TOK_DEV,), jnp.float32, 0.0, math.log(3.0)))
    position_factor = jnp.repeat(block_factor, TOK_DEV)
    noise_part = jax.random.uniform(jitter_random_key, (MEMORY_HEADS, PACKED_TOKENS), jnp.float32, -1.0, 1.0)
    step_rate = head_rate[:, None] * position_factor[None, :] * jnp.exp(noise_part)
    gate_logits = -jnp.log(jnp.expm1(step_rate))
    spike_positions = jax.random.randint(spike_random_key, (4,), 0, PACKED_TOKENS)
    spike_mask = jnp.any(jnp.arange(PACKED_TOKENS)[:, None] == spike_positions[None, :], axis=1)
    spike_height = jax.random.uniform(dropout_random_key, (MEMORY_HEADS, PACKED_TOKENS), jnp.float32, -0.4, 1.4)
    return jnp.where(spike_mask[None, :], spike_height, gate_logits)


def shard_levels(key, shape, cuts, least, largest):
    level = 1.0
    for position, shards_of in cuts:
        heights = jax.random.uniform(jax.random.fold_in(jax.random.fold_in(key, 6), position), (shards_of,), jnp.float32, least / len(cuts), largest / len(cuts))
        level = level * jnp.repeat(jnp.exp(heights), shape[position] // shards_of).reshape((-1,) + (1,) * (len(shape) - 1 - position))
    return level


def length_profile(amount, total, limit, skew):
    loads = [(1 << 20) // math.isqrt(rank ** skew) + 1 for rank in range(2, amount + 1)]
    rest, given = total - limit - (amount - 1), [1] * (amount - 1)
    while rest > 0:
        free = [i for i in range(amount - 1) if given[i] < limit]
        pool, remaining = sum([loads[i] for i in free]), rest
        for i in free:
            more = min(limit - given[i], max(1, remaining * loads[i] // pool), rest)
            given[i] = given[i] + more
            rest = rest - more
    return np.array([limit] + given)


def ragged_sizes(own_key, count, total, most, lean):
    if count == 2:
        one = jax.random.randint(own_key, (), max(1, total - most), min(most, total - 1) + 1)
        return jnp.stack([one, total - one])
    lengths = jnp.asarray(length_profile(count, total, most, lean), jnp.int32)
    twos = (count - 1) // 2
    donor, receiver = lengths[1:1 + 2 * twos:2], lengths[2:2 + 2 * twos:2]
    margin = jnp.minimum(donor - 1, most - receiver)
    moved = jax.random.randint(jax.random.fold_in(own_key, 1), (twos,), 0, 1 << 20) % (margin + 1)
    lengths = lengths.at[1:1 + 2 * twos:2].set(donor - moved).at[2:2 + 2 * twos:2].set(receiver + moved)
    return lengths[jax.random.permutation(jax.random.fold_in(own_key, 2), count)]


def gaussian(rng, dims, width, most, pieces=(), held_as=jnp.bfloat16):
    values = width * jax.random.normal(rng, dims, jnp.float32)
    if pieces:
        values = values * shard_levels(rng, dims, pieces, -0.22, 0.18)
    return jnp.clip(values, -most, most).astype(held_as)


def setup_inputs(seed: int = 0) -> dict:
    arg_keys = jax.random.split(jax.random.key(seed), 12)
    residual = gaussian(arg_keys[0], (PACKED_TOKENS, D), 1.0, 6.0, ((0, 256),))
    query_vectors = gaussian(arg_keys[1], (PACKED_TOKENS, HW), 1.0, 6.0, ((0, 64), (1, 4)))
    key_vectors = gaussian(arg_keys[2], (PACKED_TOKENS, HW), 1.0, 6.0, ((0, 64), (1, 4)))
    value_vectors = gaussian(arg_keys[3], (PACKED_TOKENS, HW), 1.0, 6.0, ((0, 64), (1, 4)))
    in_gate = draw_in_gate(jax.random.fold_in(arg_keys[11], 71), 0)
    forget_gate = draw_forget_gate(jax.random.fold_in(arg_keys[11], 71), 0)
    documents = jnp.searchsorted(jnp.cumsum(ragged_sizes(arg_keys[6], DOCS, PACKED_TOKENS, DOC_MOST, 0)), jnp.arange(PACKED_TOKENS), side="right").astype(jnp.int32)
    w_out = gaussian(arg_keys[7], (HW, D), HW ** -0.5, 0.25, ((0, 4),))
    norm_gain = jnp.clip(1.0 + 0.18 * jax.random.normal(arg_keys[8], (D,), jnp.float32), 0.099609375, 1.8984375).astype(jnp.bfloat16)
    w_up = gaussian(arg_keys[9], (D, FF), D ** -0.5, 0.125, ((0, 64), (1, 4)))
    w_down = gaussian(arg_keys[10], (FF, D), FF ** -0.5, 0.0625, ((0, 4), (1, 64)))
    return {"residual": residual, "query_vectors": query_vectors, "key_vectors": key_vectors, "value_vectors": value_vectors, "in_gate": in_gate, "forget_gate": forget_gate, "documents": documents, "w_out": w_out, "norm_gain": norm_gain, "w_up": w_up, "w_down": w_down}


very_negative = -1e+30
epsilon = 1e-06

def identity_state(head_count, head_dim):
    return (jnp.zeros((head_count, head_dim, head_dim), jnp.float32), jnp.zeros((head_count, head_dim), jnp.float32), jnp.full((head_count,), very_negative, jnp.float32), jnp.zeros((head_count,), jnp.float32), jnp.array(-1.0, jnp.float32), jnp.array(-1.0, jnp.float32))

def combine(earlier, later):
    memory_one, normal_one, top_one, decay_one, first_one, last_one = earlier
    memory_two, normal_two, top_two, decay_two, first_two, last_two = later
    later_empty = first_two < 0.0
    earlier_empty = first_one < 0.0
    keep = later_empty | (first_two == last_two) & (first_two == last_one)
    decay_step = jnp.where(later_empty, 0.0, decay_two)
    top_new = jnp.where(keep, jnp.maximum(decay_step + top_one, top_two), top_two)
    scale_old = jnp.where(keep, jnp.exp(decay_step + top_one - top_new), 0.0)
    scale_new = jnp.exp(top_two - top_new)
    memory_new = scale_old[:, None, None] * memory_one + scale_new[:, None, None] * memory_two
    normal_new = scale_old[:, None] * normal_one + scale_new[:, None] * normal_two
    decay_new = jnp.where(keep, decay_one + decay_step, decay_two)
    first_new = jnp.where(earlier_empty, first_two, first_one)
    last_new = jnp.where(later_empty, last_one, last_two)
    return (memory_new, normal_new, top_new, decay_new, first_new, last_new)

def block_summary(key_block, value_block, gate_block, decay_block, segment):
    cumulative = jnp.cumsum(decay_block, axis=-1)
    latest = segment == segment[-1]
    growth = jnp.where(latest[None, :], cumulative[:, -1:] - cumulative + gate_block, very_negative)
    top_log = lax.optimization_barrier(jnp.max(growth, axis=-1))
    weight_table = jnp.exp(growth - top_log[:, None])
    key_expanded = key_block.astype(jnp.float32)
    value_expanded = value_block.astype(jnp.float32)
    memory_matrix = jnp.einsum('jw,wjm,wju->jmu', weight_table, key_expanded, value_expanded, precision=lax.Precision.HIGHEST)
    normal = jnp.einsum('hs,shk->hk', weight_table, key_expanded, precision=lax.Precision.HIGHEST)
    return (memory_matrix, normal, top_log, cumulative[:, -1], segment[0], segment[-1])

def block_output(query_block, key_block, value_block, gate_block, decay_block, segment, state):
    memory_matrix, normal, top_log, total_decay, first_doc, last_doc = state
    head_dim = query_block.shape[2]
    length = segment.shape[0]
    cumulative = jnp.cumsum(decay_block, axis=-1)
    row_ids = lax.broadcasted_iota(jnp.int32, (length, length), 0)
    col_ids = lax.broadcasted_iota(jnp.int32, (length, length), 1)
    allowed = (col_ids <= row_ids) & (segment[:, None] == segment[None, :])
    inside = jnp.where(allowed[None], cumulative[:, :, None] - cumulative[:, None, :] + gate_block[:, None, :], very_negative)
    outside = jnp.where((segment == last_doc)[None, :], cumulative + top_log[:, None], very_negative)
    peak_log = jnp.maximum(outside, lax.optimization_barrier(jnp.max(inside, axis=-1)))
    carried = jnp.exp(outside - peak_log)
    scaled_expanded = query_block.astype(jnp.float32) * head_dim ** (-0.5)
    scores = jnp.einsum('lhd,shd->hls', scaled_expanded, key_block.astype(jnp.float32))
    weight_table = jnp.exp(inside - peak_log[:, :, None]) * scores
    rounded = lax.optimization_barrier(weight_table.astype(jnp.bfloat16))
    from_block = jnp.einsum('hls,shv->hlv', rounded.astype(jnp.float32), value_block.astype(jnp.float32))
    memory_readout = jnp.einsum('pug,uga->upa', scaled_expanded, memory_matrix, precision=lax.Precision.HIGHEST)
    numer_part = carried[:, :, None] * memory_readout + from_block
    denom_part = carried * jnp.einsum('lhk,hk->hl', scaled_expanded, normal, precision=lax.Precision.HIGHEST) + lax.optimization_barrier(jnp.sum(weight_table, axis=-1))
    result = numer_part / jnp.maximum(jnp.abs(denom_part), jnp.exp(-peak_log))[:, :, None]
    return jnp.transpose(result, (1, 0, 2)).reshape(length, -1).astype(jnp.bfloat16)

def reference(residual, query_vectors, key_vectors, value_vectors, in_gate, forget_gate, documents, w_out, norm_gain, w_up, w_down):
    head_count = in_gate.shape[0]
    head_dim = query_vectors.shape[1] // head_count
    total_rows = query_vectors.shape[0]
    block_count = total_rows // SPAN

    def to_blocks(vectors):
        return vectors.reshape(block_count, SPAN, head_count, head_dim)

    def gate_blocks(gates):
        return jnp.transpose(gates.reshape(head_count, block_count, SPAN), (1, 0, 2))
    segments = documents.astype(jnp.float32).reshape(block_count, SPAN)
    inputs_all = (to_blocks(query_vectors), to_blocks(key_vectors), to_blocks(value_vectors), gate_blocks(in_gate), gate_blocks(jax.nn.log_sigmoid(forget_gate)), segments)

    def block_step(state, inputs):
        query_block, key_block, value_block, gate_block, decay_block, segment = inputs
        output = block_output(query_block, key_block, value_block, gate_block, decay_block, segment, state)
        summary = block_summary(key_block, value_block, gate_block, decay_block, segment)
        return (combine(state, summary), output)
    _, mixed = lax.scan(block_step, identity_state(head_count, head_dim), inputs_all)
    mixed = mixed.reshape(total_rows, head_count * head_dim)
    group_width = w_up.shape[1] // N_TP

    def row_block(inputs):
        mixed_rows, residual_rows = inputs
        projected = jnp.dot(mixed_rows, w_out, preferred_element_type=jnp.float32)
        middle = (residual_rows.astype(jnp.float32) + projected).astype(jnp.bfloat16)
        middle_wide = middle.astype(jnp.float32)
        factor = lax.rsqrt(lax.optimization_barrier(jnp.mean(middle_wide * middle_wide, axis=-1, keepdims=True)) + epsilon)
        normed = (middle_wide * factor * norm_gain.astype(jnp.float32)).astype(jnp.bfloat16)
        lifted = jnp.dot(normed, w_up, preferred_element_type=jnp.float32)
        hidden = jnp.square(jax.nn.relu(lifted)).astype(jnp.bfloat16)
        summed = jnp.zeros(middle.shape, jnp.float32)
        for column_group in range(N_TP):
            lower = column_group * group_width
            partial_sum = jnp.dot(hidden[:, lower:lower + group_width], w_down[lower:lower + group_width], preferred_element_type=jnp.float32)
            rounded = lax.optimization_barrier(partial_sum.astype(jnp.bfloat16))
            summed = summed + rounded.astype(jnp.float32)
        return (middle_wide + summed).astype(jnp.bfloat16)
    blocks_out = lax.map(row_block, (mixed.reshape(-1, TOK_DEV, head_count * head_dim), residual.reshape(-1, TOK_DEV, residual.shape[1])))
    return blocks_out.reshape(residual.shape)
```

```python
import functools

import jax
import jax.numpy as jnp
from jax import lax
from jax.experimental import pallas as pl
from jax.experimental.pallas import tpu as pltpu
from jax.sharding import Mesh
from jax.sharding import PartitionSpec as P


SP = ("sp_0", "sp_1", "sp_2")
SP_TP = ("sp_0", "sp_1", "sp_2", "tp")
Z, X, C, Y = SP_TP
CHIPS_BACK = 4
very_negative = -1e30
epsilon = 1e-06
f32 = jnp.float32
bf16 = jnp.bfloat16
HIGH = lax.Precision.HIGHEST

VM = pl.BlockSpec(memory_space=pltpu.VMEM)
SM = pl.BlockSpec(memory_space=pltpu.SMEM)
ANY = pl.BlockSpec(memory_space=pl.ANY)


def call(kernel, outs, ins, args, scratch=(), flops=1, traffic=1, vmem=16):
    many = isinstance(outs, (list, tuple))
    return pl.pallas_call(
        kernel,
        out_shape=outs,
        in_specs=ins,
        out_specs=[VM] * len(outs) if many else VM,
        scratch_shapes=list(scratch),
        cost_estimate=pl.CostEstimate(flops=flops, bytes_accessed=traffic, transcendentals=0),
        compiler_params=pltpu.CompilerParams(vmem_limit_bytes=vmem * 1024 * 1024),
    )(*args)


def halves(shape, zero, one):
    lane = lax.broadcasted_iota(jnp.int32, shape, 1)
    return jnp.where(lane < 64, zero, one)


def copy_all(pairs, sems):
    copies = [pltpu.make_async_copy(a, b, sems.at[k]) for k, (a, b) in enumerate(pairs)]
    for c in copies:
        c.start()
    for c in copies:
        c.wait()


def at(start, size):
    return pl.ds(pl.multiple_of(start, size), size)


STATE_ROWS = 72


def state_kernel(*refs):
    (state, rows, columns), (in_gate, forget_gate, docs, keys, values), sems = refs[5:8], refs[8:13], refs[13]
    copy_all(list(zip(refs[:5], refs[8:13])), sems)
    forget = forget_gate[...]
    decay = jnp.minimum(forget, 0.0) - jnp.log1p(jnp.exp(-jnp.abs(forget)))
    lane = lax.broadcasted_iota(jnp.int32, decay.shape, 1)
    total = decay
    step = 1
    while step < decay.shape[1]:
        total = total + jnp.where(lane >= step, pltpu.roll(total, step, 1), 0.0)
        step *= 2
    gate = in_gate[...]
    doc = docs[...].astype(f32)
    table = jnp.concatenate([total, gate, doc, jnp.zeros((3, doc.shape[1]), f32)], axis=0)
    rows[...] = table
    turned = jnp.transpose(table)
    columns[...] = turned
    last = doc[:, -1:]
    end = total[:, -1:]
    growth = jnp.where(doc == last, end - total + gate, very_negative)
    top = jnp.max(growth, axis=1, keepdims=True)
    latest = turned[:, 4:5] == last
    weight = []
    for h in range(2):
        grown = jnp.where(latest, end[h:h + 1] - turned[:, h:h + 1] + turned[:, 2 + h:3 + h], very_negative)
        weight.append(jnp.exp(grown - top[h:h + 1]))
    wide = halves(keys.shape, weight[0], weight[1])
    weighted = wide * keys[...].astype(f32)
    full = jnp.dot(jnp.transpose(weighted), values[...].astype(f32), precision=HIGH, preferred_element_type=f32)
    state[0:64, :] = halves((64, 128), full[0:64], full[64:128])
    normal = jnp.sum(weighted, axis=0, keepdims=True)
    tail = [
        normal,
        halves((1, 128), top[0:1], top[1:2]),
        halves((1, 128), end[0:1], end[1:2]),
        jnp.broadcast_to(last, (1, 128)),
        jnp.zeros((4, 128), f32),
    ]
    state[64:72, :] = jnp.concatenate(tail, axis=0)


def local_kernel(rows, columns, *refs):
    (numer, denom, peak), (queries, keys, values), sems = refs[3:6], refs[6:9], refs[9]
    copy_all(list(zip(refs[:3], refs[6:9])), sems)
    length = queries.shape[0]
    scaled = queries[...] * jnp.asarray(0.125, bf16)
    key = keys[...]
    value = values[...]
    row_ids = lax.broadcasted_iota(jnp.int32, (length, length), 0)
    col_ids = lax.broadcasted_iota(jnp.int32, (length, length), 1)
    allowed = (col_ids <= row_ids) & (columns[:, 4:5] == rows[4:5, :])
    found = []
    for h in range(2):
        inside = jnp.where(
            allowed,
            columns[:, h:h + 1] - rows[h:h + 1, :] + rows[2 + h:3 + h, :],
            very_negative,
        )
        top = jnp.max(inside, axis=1, keepdims=True)
        mine = halves(key.shape, jnp.asarray(1 - h, bf16), jnp.asarray(h, bf16)) * key
        scores = lax.dot_general(scaled, mine, (((1,), (1,)), ((), ())), preferred_element_type=f32)
        weight = jnp.exp(inside - top) * scores
        summed = jnp.dot(weight.astype(bf16), value, preferred_element_type=f32)
        found.append((summed, jnp.sum(weight, axis=1, keepdims=True), top))
    numer[...] = halves(numer.shape, found[0][0], found[1][0])
    denom[...] = halves(denom.shape, found[0][1], found[1][1])
    peak[...] = halves(peak.shape, found[0][2], found[1][2])


def merge_kernel(columns, numer, denom, peak, *refs):
    count = CHIPS_BACK + 2
    mixed, sems = refs[count], refs[2 * count + 1]
    copy_all(list(zip(refs[:count], refs[count + 1:2 * count + 1])), sems)
    queries, received, other = refs[count + 1], refs[count + 2:2 * count], refs[2 * count]
    c = lax.axis_index(C)
    chip = lax.axis_index(Z) * 4 + lax.axis_index(X)
    upper = jnp.zeros((1, 128), jnp.int32) + c == 1
    chips = jnp.zeros((1, 128), jnp.int32) + chip
    states = [(other[0:STATE_ROWS], upper)]
    for back in range(1, CHIPS_BACK + 1):
        mine = received[back - 1][...]
        theirs = other[back * STATE_ROWS:(back + 1) * STATE_ROWS]
        states.append((jnp.where(c == 1, mine, theirs), chips >= back))
        states.append((jnp.where(c == 1, theirs, mine), chips >= back))
    open_doc = jnp.where(upper, states[0][0][67:68], states[1][0][67:68])
    decayed = jnp.zeros((1, 128), f32)
    reach = []
    for state, there in states:
        joined = (state[67:68] == open_doc) & there
        reach.append(jnp.where(joined, state[65:66] + decayed, very_negative))
        decayed = decayed + jnp.where(there, state[66:67], 0.0)
    top = functools.reduce(jnp.maximum, reach)
    memory = jnp.zeros((64, 128), f32)
    normal = jnp.zeros((1, 128), f32)
    for far, (state, _) in zip(reach, states):
        scale = jnp.where(far > 0.5 * very_negative, jnp.exp(far - top), 0.0)
        memory = memory + scale * state[0:64]
        normal = normal + scale * state[64:65]
    open_here = (columns[:, 4:5] == open_doc) & (top > 0.5 * very_negative)
    moved = halves(peak.shape, columns[:, 0:1], columns[:, 1:2])
    outside = jnp.where(open_here, moved + top, very_negative)
    inner = peak[...]
    both = jnp.maximum(outside, inner)
    carried = jnp.exp(outside - both)
    kept = jnp.exp(inner - both)
    scaled = queries[...].astype(f32) * 0.125
    blocks = jnp.concatenate([halves((64, 128), memory, 0.0), halves((64, 128), 0.0, memory)], axis=0)
    readout = jnp.dot(scaled, blocks, precision=HIGH, preferred_element_type=f32)
    ones = jnp.concatenate([halves((64, 128), 1.0, 0.0), halves((64, 128), 0.0, 1.0)], axis=0)
    along = jnp.dot(scaled * normal, ones, precision=HIGH, preferred_element_type=f32)
    top_part = kept * numer[...] + carried * readout
    low_part = kept * denom[...] + carried * along
    mixed[...] = (top_part / jnp.maximum(jnp.abs(low_part), jnp.exp(-both))).astype(bf16)


def middle_kernel(early_own, early_other, gain, *refs):
    pieces, (middle, normed, weights, residual, heads, sems) = refs[:8], refs[8:]
    c, y = lax.axis_index(C), lax.axis_index(Y)
    pairs = []
    for core, early in ((0, early_own), (1, early_other)):
        for k in range(4):
            there = (y + k) % 4
            row = (core * 4 + k) * 64
            pairs.append((early.at[there, 0:64], residual.at[row:row + 64]))
            weight_row = there * 128 + (c + core) % 2 * 64
            pairs.append((early.at[there, 64:128], weights.at[at(weight_row, 64)]))
    for core in range(2):
        for back in range(4):
            piece = pieces[core * 4 + back]
            lanes = at((y + 4 - back) % 4 * 128, 128)
            for k in range(4):
                row = (core * 4 + k) * 64
                pairs.append((piece.at[at((y + k) % 4 * 64, 64)], heads.at[row:row + 64, lanes]))
    copy_all(pairs, sems)

    def rows(t, carry):
        part = at(t * 128, 128)
        projected = jnp.dot(heads[part, :], weights[...], preferred_element_type=f32)
        mid = (residual[part, :].astype(f32) + projected).astype(bf16)
        middle[part, :] = mid
        wide = mid.astype(f32)
        factor = lax.rsqrt(jnp.mean(wide * wide, axis=1, keepdims=True) + epsilon)
        normed[part, :] = (wide * factor * gain[...].astype(f32)).astype(bf16)
        return carry

    lax.fori_loop(0, 4, rows, 0)


OFFSETS = (0, -1, 1, -2, 2, -3, 3, -4)
X_OFFSETS = (0, -1, 1, 2)


def up_kernel(slots, first, final, normed, *refs):
    units = refs[:len(slots) + final]
    refs = refs[len(slots) + final:]
    before, (out, weights, total, sems) = (None, refs) if first else (refs[0], refs[1:])
    z, x = lax.axis_index(Z), lax.axis_index(X)
    waits = []
    for j in range(len(slots)):
        copies = []
        for k, offset in enumerate(X_OFFSETS):
            row = j * 256 + (x + 4 + offset) % 4 * 64
            unit, start = (units[k // 2], k % 2 * 64) if final else (units[j], k * 64)
            copies.append(
                pltpu.make_async_copy(unit.at[start:start + 64], weights.at[at(row, 64)], sems.at[j * 4 + k])
            )
            copies[-1].start()
        waits.append(copies)
    if not first:
        load = pltpu.make_async_copy(before, total, sems.at[4 * len(slots)])
        load.start()
    for j, slot in enumerate(slots):
        for copy in waits[j]:
            copy.wait()
        if j == 0 and not first:
            load.wait()
        lanes = at((z + 8 + OFFSETS[slot]) % 8 * 256, 256)
        for n in range(4):
            part = slice(n * 256, n * 256 + 256)
            term = jnp.dot(normed[:, lanes], weights[j * 256:j * 256 + 256, part], preferred_element_type=f32)
            if j or not first:
                term = term + total[:, part]
            if j + 1 < len(slots):
                total[:, part] = term
            elif final:
                positive = jnp.maximum(term, 0.0)
                out[:, part] = (positive * positive).astype(bf16)
            else:
                out[:, part] = term


def gather_kernel(rows, *refs):
    pieces, out, sems = refs[:-2], refs[-2], refs[-1]
    copy_all([(p, out.at[k * rows:(k + 1) * rows]) for k, p in enumerate(pieces)], sems)


def down_kernel(other_half, hidden_in, mine, before, after, far_a, far_b, *refs):
    if other_half:
        partial, refs = refs[0], refs[1:]
        outs, (weights, hidden, total, sems) = refs[:8], refs[8:]
    else:
        out, weights, hidden, sems = refs
    c, z, x = lax.axis_index(C), lax.axis_index(Z), lax.axis_index(X)
    lanes = at((1 - c if other_half else c) * 1024, 1024)
    loads = []
    if other_half:
        loads.append(pltpu.make_async_copy(hidden_in.at[256:512], hidden.at[0:256], sems.at[32]))
        loads.append(pltpu.make_async_copy(hidden_in.at[0:256], hidden.at[256:512], sems.at[33]))
        loads.append(pltpu.make_async_copy(partial, total, sems.at[34]))
    else:
        loads.append(pltpu.make_async_copy(hidden_in, hidden, sems.at[32]))
    copies = []
    for slot in range(8):
        for k, (source, offset) in enumerate(((mine, 0), (before, -1), (after, 1), (None, 2))):
            row = slot * 32
            if source is None:
                source, row = (far_a, row) if slot < 4 else (far_b, row - 128)
            to = at(slot * 128 + (x + 4 + offset) % 4 * 32, 32)
            copies.append(
                pltpu.make_async_copy(source.at[row:row + 32, lanes], weights.at[to], sems.at[slot * 4 + k])
            )
    for copy in loads + copies:
        copy.start()
    for copy in loads:
        copy.wait()
    for n in range(4):
        for copy in copies[8 * n:8 * n + 8]:
            copy.wait()
        part = slice(n * 256, n * 256 + 256)
        terms = lax.dot_general(
            hidden[...], weights[part, :], (((1,), (1,)), ((), ())), preferred_element_type=f32
        )
        if not other_half:
            out[:, part] = terms
            continue
        terms = (terms + total[:, part]).astype(bf16)
        for half in range(2):
            to = at((z + 8 + OFFSETS[2 * n + half]) % 8 * 128, 128)
            for k in range(8):
                outs[k][:, to] = terms[k * 64:k * 64 + 64, half * 128:half * 128 + 128]


def last_kernel(*refs):
    out, middle, terms, stacked, sems = refs[9], refs[10], refs[11], refs[12], refs[13]
    c = lax.axis_index(C)
    copy_all([(refs[0].at[0:64], middle)] + [(refs[1 + k], terms.at[k]) for k in range(8)], sems)
    for core in range(2):
        lanes = at((c + core) % 2 * 256, 256)
        for k in range(4):
            for b in range(4):
                row = (b * 4 + k) * 64
                stacked[row:row + 64, lanes] = terms[core * 4 + k, :, b * 256:b * 256 + 256]
    s = lax.broadcasted_iota(jnp.int32, (512, 512), 0)
    d = lax.broadcasted_iota(jnp.int32, (512, 512), 1)
    wanted = ((s % 256) // 32) * 64 + (s // 256) * 32 + s % 32
    turn = (wanted == d).astype(f32).astype(bf16)
    for b in range(4):
        spread = jnp.dot(stacked[b * 256:b * 256 + 256, :], turn, preferred_element_type=f32)
        summed = spread[0:64] + spread[64:128] + spread[128:192] + spread[192:256]
        part = slice(b * 512, b * 512 + 512)
        out[:, part] = (middle[:, part].astype(f32) + summed).astype(bf16)


def shift(value, axis, by):
    n = lax.axis_size(axis)
    return lax.ppermute(value, axis, [(i, (i + by) % n) for i in range(n)])


def to_peer(value, core, by):
    pairs = [(c * 4 + y, (c ^ core) * 4 + (y + by) % 4) for c in range(2) for y in range(4)]
    return lax.ppermute(value, (C, Y), pairs)


def z_ring(piece, steps=4):
    up, down = [piece], [piece]
    for step in range(steps):
        up.append(shift(up[-1], Z, 1))
        if step < 3:
            down.append(shift(down[-1], Z, -1))
    return [piece, up[1], down[1], up[2], down[2], up[3], down[3], *up[4:]]


def layer(
    residual,
    query_vectors,
    key_vectors,
    value_vectors,
    in_gate,
    forget_gate,
    documents,
    w_out,
    norm_gain,
    w_up,
    w_down,
):
    c = lax.axis_index(C)
    first = c == 0
    left, right = w_up[:, :1024], w_up[:, 1024:]
    keep, give = jnp.where(first, left, right), jnp.where(first, right, left)
    taken = shift(give, C, 1)
    mine = jnp.where(
        first, jnp.concatenate([keep, taken], axis=0), jnp.concatenate([taken, keep], axis=0)
    )
    across = [mine, shift(mine, X, 1), shift(mine, X, -1), shift(mine, X, 2)]
    unit = call(
        functools.partial(gather_kernel, 64),
        jax.ShapeDtypeStruct((256, 1024), bf16),
        [ANY] * 4,
        across,
        scratch=[pltpu.SemaphoreType.DMA((4,))],
        flops=1_000_000,
        vmem=4,
    )
    up_units = z_ring(unit, 3)
    far_up = shift(up_units[5][:128], Z, 1)
    far_down = shift(up_units[6][128:], Z, -1)
    down_columns = call(
        functools.partial(gather_kernel, 32),
        jax.ShapeDtypeStruct((256, 2048), bf16),
        [ANY] * 8,
        z_ring(w_down.T),
        scratch=[pltpu.SemaphoreType.DMA((8,))],
        flops=1_000_000,
        vmem=4,
    )
    before, after = shift(down_columns, X, 1), shift(down_columns, X, -1)
    far_a = shift(before[:128], X, 1)
    far_b = shift(after[128:], X, -1)
    docs = documents.reshape(1, -1)
    tokens = query_vectors.shape[0]
    wide = jax.ShapeDtypeStruct((tokens, 128), f32)
    state, rows, columns = call(
        state_kernel,
        [
            jax.ShapeDtypeStruct((STATE_ROWS, 128), f32),
            jax.ShapeDtypeStruct((8, tokens), f32),
            jax.ShapeDtypeStruct((tokens, 8), f32),
        ],
        [ANY] * 5,
        (in_gate, forget_gate, docs, key_vectors, value_vectors),
        scratch=[
            pltpu.VMEM(in_gate.shape, f32),
            pltpu.VMEM(in_gate.shape, f32),
            pltpu.VMEM(docs.shape, jnp.int32),
            pltpu.VMEM((tokens, 128), bf16),
            pltpu.VMEM((tokens, 128), bf16),
            pltpu.SemaphoreType.DMA((5,)),
        ],
        flops=50_000_000,
    )
    received = [
        lax.ppermute(state, (Z, X), [(i, (i + back) % 32) for i in range(32)])
        for back in range(1, CHIPS_BACK + 1)
    ]
    states = call(
        functools.partial(gather_kernel, STATE_ROWS),
        jax.ShapeDtypeStruct((STATE_ROWS * (CHIPS_BACK + 1), 128), f32),
        [ANY] * (CHIPS_BACK + 1),
        (state, *received),
        scratch=[pltpu.SemaphoreType.DMA((CHIPS_BACK + 1,))],
        flops=1_000_000,
        vmem=4,
    )
    other = shift(states, C, 1)
    numer, denom, peak = call(
        local_kernel,
        [wide] * 3,
        [VM] * 2 + [ANY] * 3,
        (rows, columns, query_vectors, key_vectors, value_vectors),
        scratch=[pltpu.VMEM((tokens, 128), bf16)] * 3 + [pltpu.SemaphoreType.DMA((3,))],
        flops=100_000_000,
    )
    out_half = jnp.where(first, w_out[:64], w_out[64:])
    early = jnp.concatenate([residual, out_half], axis=0)
    early, _ = lax.optimization_barrier((early, unit))
    early_own = lax.all_to_all(jnp.broadcast_to(early[None], (4, 128, 2048)), Y, 0, 0, tiled=True)
    early_other = shift(early_own, C, 1)
    mixed = call(
        merge_kernel,
        jax.ShapeDtypeStruct((tokens, 128), bf16),
        [VM] * 4 + [ANY] * (2 + CHIPS_BACK),
        (columns, numer, denom, peak, query_vectors, *received, other),
        scratch=[
            pltpu.VMEM((tokens, 128), bf16),
            *[pltpu.VMEM((STATE_ROWS, 128), f32)] * CHIPS_BACK,
            pltpu.VMEM((STATE_ROWS * (CHIPS_BACK + 1), 128), f32),
            pltpu.SemaphoreType.DMA((CHIPS_BACK + 2,)),
        ],
        flops=100_000_000,
    )
    peers = [(core, by) for core in range(2) for by in range(4)]
    mixes = [mixed] + [to_peer(mixed, *peer) for k, peer in enumerate(peers) if k]
    rows_here = jax.ShapeDtypeStruct((512, 2048), bf16)
    middle, normed = call(
        middle_kernel,
        [rows_here] * 2,
        [ANY] * 2 + [VM] + [ANY] * 8,
        (early_own, early_other, norm_gain.reshape(1, -1), *mixes),
        scratch=[
            pltpu.VMEM((512, 2048), bf16),
            pltpu.VMEM((512, 2048), bf16),
            pltpu.VMEM((512, 512), bf16),
            pltpu.SemaphoreType.DMA((48,)),
        ],
        flops=2 * 512 * 512 * 2048,
    )
    summed = ()
    groups = ((0, 1, 2), (3, 4), (5, 6), (7,))
    for g, slots in enumerate(groups):
        final = g + 1 == len(groups)
        summed = (
            call(
                functools.partial(up_kernel, slots, g == 0, final),
                jax.ShapeDtypeStruct((512, 1024), bf16 if final else f32),
                [VM] + [ANY] * (len(slots) + final + (g > 0)),
                (normed, *([far_up, far_down] if final else [up_units[s] for s in slots]), *summed),
                scratch=[
                    pltpu.VMEM((256 * len(slots), 1024), bf16),
                    pltpu.VMEM((512, 1024), f32),
                    pltpu.SemaphoreType.DMA((4 * len(slots) + 1,)),
                ],
                flops=2 * 512 * 1024 * 256 * len(slots),
            ),
        )
    hidden = summed[0]
    hidden_other = shift(hidden, C, 1)
    pieces = (down_columns, before, after, far_a, far_b)
    space = [pltpu.VMEM((1024, 1024), bf16), pltpu.VMEM((512, 1024), bf16)]
    partial = call(
        functools.partial(down_kernel, False),
        jax.ShapeDtypeStruct((512, 1024), f32),
        [ANY] * 6,
        (hidden, *pieces),
        scratch=[*space, pltpu.SemaphoreType.DMA((33,))],
        flops=512 * 1024 * 2048,
    )
    sent = call(
        functools.partial(down_kernel, True),
        [jax.ShapeDtypeStruct((64, 1024), bf16)] * 8,
        [ANY] * 7,
        (hidden_other, *pieces, partial),
        scratch=[*space, pltpu.VMEM((512, 1024), f32), pltpu.SemaphoreType.DMA((35,))],
        flops=512 * 1024 * 2048,
    )
    terms = [sent[0]] + [to_peer(sent[k], *peer) for k, peer in enumerate(peers) if k]
    return call(
        last_kernel,
        jax.ShapeDtypeStruct((64, 2048), bf16),
        [ANY] * 9,
        (middle, *terms),
        scratch=[
            pltpu.VMEM((64, 2048), bf16),
            pltpu.VMEM((8, 64, 1024), bf16),
            pltpu.VMEM((1024, 512), bf16),
            pltpu.SemaphoreType.DMA((9,)),
        ],
        flops=2 * 1024 * 512 * 512,
    )


def solution(mesh):
    torus = Mesh(mesh.devices.reshape(8, 4, 2, mesh.shape["tp"]), SP_TP)
    in_specs = (
        P(SP_TP, None),
        P(SP, "tp"),
        P(SP, "tp"),
        P(SP, "tp"),
        P("tp", SP),
        P("tp", SP),
        P(SP),
        P("tp", None),
        P(),
        P(SP, "tp"),
        P("tp", SP),
    )
    out_specs = P(SP_TP, None)
    return jax.shard_map(layer, mesh=torus, in_specs=in_specs, out_specs=out_specs, check_vma=False)
```

```python
import functools

import jax
import jax.numpy as jnp
from jax import lax
from jax.experimental import pallas as pl
from jax.experimental.pallas import tpu as pltpu
from jax.sharding import Mesh
from jax.sharding import PartitionSpec as P


SP = ("sp_0", "sp_1", "sp_2")
SP_TP = ("sp_0", "sp_1", "sp_2", "tp")
Z, X, C, Y = SP_TP
CHIPS_BACK = 4
very_negative = -1e30
epsilon = 1e-06
f32 = jnp.float32
bf16 = jnp.bfloat16
HIGH = lax.Precision.HIGHEST

VM = pl.BlockSpec(memory_space=pltpu.VMEM)
SM = pl.BlockSpec(memory_space=pltpu.SMEM)
ANY = pl.BlockSpec(memory_space=pl.ANY)
HBM = pl.BlockSpec(memory_space=pltpu.HBM)


def call(kernel, outs, ins, args, scratch=(), flops=1, traffic=1, vmem=16):
    many = isinstance(outs, (list, tuple))
    return pl.pallas_call(
        kernel,
        out_shape=outs,
        in_specs=ins,
        out_specs=[VM] * len(outs) if many else VM,
        scratch_shapes=list(scratch),
        cost_estimate=pl.CostEstimate(flops=flops, bytes_accessed=traffic, transcendentals=0),
        compiler_params=pltpu.CompilerParams(vmem_limit_bytes=vmem * 1024 * 1024),
    )(*args)


def halves(shape, zero, one):
    lane = lax.broadcasted_iota(jnp.int32, shape, 1)
    return jnp.where(lane < 64, zero, one)


def copy_all(pairs, sems):
    copies = [pltpu.make_async_copy(a, b, sems.at[k]) for k, (a, b) in enumerate(pairs)]
    for c in copies:
        c.start()
    for c in copies:
        c.wait()


def at(start, size):
    return pl.ds(pl.multiple_of(start, size), size)


STATE_ROWS = 72


def memory_kernel(*refs):
    state, packed = refs[6:8]
    in_gate, forget_gate, docs, queries, keys, values = refs[8:14]
    copy_all(list(zip(refs[:6], refs[8:14])), refs[14])
    forget = forget_gate[...]
    decay = jnp.minimum(forget, 0.0) - jnp.log1p(jnp.exp(-jnp.abs(forget)))
    lane = lax.broadcasted_iota(jnp.int32, decay.shape, 1)
    total = decay
    step = 1
    while step < decay.shape[1]:
        total = total + jnp.where(lane >= step, pltpu.roll(total, step, 1), 0.0)
        step *= 2
    gate = in_gate[...]
    doc = docs[...].astype(f32)
    table = jnp.concatenate([total, gate, doc, jnp.zeros((3, doc.shape[1]), f32)], axis=0)
    turned = jnp.transpose(table)
    last = doc[:, -1:]
    end = total[:, -1:]
    growth = jnp.where(doc == last, end - total + gate, very_negative)
    top = jnp.max(growth, axis=1, keepdims=True)
    latest = turned[:, 4:5] == last
    weight = []
    for h in range(2):
        grown = jnp.where(latest, end[h:h + 1] - turned[:, h:h + 1] + turned[:, 2 + h:3 + h], very_negative)
        weight.append(jnp.exp(grown - top[h:h + 1]))
    wide = halves(keys.shape, weight[0], weight[1])
    weighted = wide * keys[...].astype(f32)
    full = jnp.dot(jnp.transpose(weighted), values[...].astype(f32), precision=HIGH, preferred_element_type=f32)
    state[0:64, :] = halves((64, 128), full[0:64], full[64:128])
    normal = jnp.sum(weighted, axis=0, keepdims=True)
    tail = [
        normal,
        halves((1, 128), top[0:1], top[1:2]),
        halves((1, 128), end[0:1], end[1:2]),
        jnp.broadcast_to(last, (1, 128)),
        jnp.zeros((4, 128), f32),
    ]
    state[64:72, :] = jnp.concatenate(tail, axis=0)

    length = queries.shape[0]
    scaled = queries[...] * jnp.asarray(0.125, bf16)
    key = keys[...]
    value = values[...]
    row_ids = lax.broadcasted_iota(jnp.int32, (length, length), 0)
    col_ids = lax.broadcasted_iota(jnp.int32, (length, length), 1)
    allowed = (col_ids <= row_ids) & (turned[:, 4:5] == doc)
    found = []
    for h in range(2):
        inside = jnp.where(
            allowed,
            turned[:, h:h + 1] - total[h:h + 1, :] + gate[h:h + 1, :],
            very_negative,
        )
        peak = jnp.max(inside, axis=1, keepdims=True)
        mine = halves(key.shape, jnp.asarray(1 - h, bf16), jnp.asarray(h, bf16)) * key
        scores = lax.dot_general(scaled, mine, (((1,), (1,)), ((), ())), preferred_element_type=f32)
        weight = jnp.exp(inside - peak) * scores
        summed = jnp.dot(weight.astype(bf16), value, preferred_element_type=f32)
        found.append((summed, jnp.sum(weight, axis=1, keepdims=True), peak, turned[:, h:h + 1]))
    for k in range(4):
        packed[:, k * 128:k * 128 + 128] = halves((length, 128), found[0][k], found[1][k])
    packed[:, 512:640] = jnp.broadcast_to(turned[:, 4:5], (length, 128))
    packed[:, 640:768] = scaled.astype(f32)


def merge_kernel(packed, states_own, other, mixed):
    numer, denom, inner, moved, doc, scaled = (packed[:, k * 128:k * 128 + 128] for k in range(6))
    c = lax.axis_index(C)
    chip = lax.axis_index(Z) * 4 + lax.axis_index(X)
    upper = jnp.zeros((1, 128), jnp.int32) + c == 1
    chips = jnp.zeros((1, 128), jnp.int32) + chip
    states = [(other[0:STATE_ROWS], upper)]
    for back in range(1, CHIPS_BACK + 1):
        there = slice(back * STATE_ROWS, (back + 1) * STATE_ROWS)
        mine, theirs = states_own[there], other[there]
        states.append((jnp.where(c == 1, mine, theirs), chips >= back))
        states.append((jnp.where(c == 1, theirs, mine), chips >= back))
    open_doc = jnp.where(upper, states[0][0][67:68], states[1][0][67:68])
    decayed = jnp.zeros((1, 128), f32)
    reach = []
    for state, there in states:
        joined = (state[67:68] == open_doc) & there
        reach.append(jnp.where(joined, state[65:66] + decayed, very_negative))
        decayed = decayed + jnp.where(there, state[66:67], 0.0)
    top = functools.reduce(jnp.maximum, reach)
    memory = jnp.zeros((64, 128), f32)
    normal = jnp.zeros((1, 128), f32)
    for far, (state, _) in zip(reach, states):
        scale = jnp.where(far > 0.5 * very_negative, jnp.exp(far - top), 0.0)
        memory = memory + scale * state[0:64]
        normal = normal + scale * state[64:65]
    open_here = (doc == open_doc) & (top > 0.5 * very_negative)
    outside = jnp.where(open_here, moved + top, very_negative)
    both = jnp.maximum(outside, inner)
    carried = jnp.exp(outside - both)
    kept = jnp.exp(inner - both)
    blocks = jnp.concatenate([halves((64, 128), memory, 0.0), halves((64, 128), 0.0, memory)], axis=0)
    readout = jnp.dot(scaled, blocks, precision=HIGH, preferred_element_type=f32)
    ones = jnp.concatenate([halves((64, 128), 1.0, 0.0), halves((64, 128), 0.0, 1.0)], axis=0)
    along = jnp.dot(scaled * normal, ones, precision=HIGH, preferred_element_type=f32)
    top_part = kept * numer + carried * readout
    low_part = kept * denom + carried * along
    result = (top_part / jnp.maximum(jnp.abs(low_part), jnp.exp(-both))).astype(bf16)
    mixed[...] = result


def early_kernel(residual, w_out, out, sems):
    rows = at(lax.axis_index(C) * 64, 64)
    copy_all(
        [(residual, out.at[k, 0:64]) for k in range(4)]
        + [(w_out.at[rows], out.at[k, 64:128]) for k in range(4)],
        sems,
    )


def middle_kernel(early_own, early_other, gain, mixes_own, mixes_other, middle, normed, weights, heads, projected):
    c, y = lax.axis_index(C), lax.axis_index(Y)
    for core, early in ((0, early_own), (1, early_other)):
        for there in range(4):
            row = at(there * 128 + (c + core) % 2 * 64, 64)
            weights[row, :] = early[there, 64:128, :]
    for core, mixes in ((0, mixes_own), (1, mixes_other)):
        for back in range(4):
            lanes = at((y + 4 - back) % 4 * 128, 128)
            for k in range(4):
                row = (core * 4 + k) * 64
                heads[row:row + 64, lanes] = mixes[at(back * 256 + (y + k) % 4 * 64, 64), :]

    def columns(n, carry):
        part = at(n * 256, 256)
        projected[:, part] = jnp.dot(heads[...], weights[:, part], preferred_element_type=f32)
        return carry

    lax.fori_loop(0, 8, columns, 0, unroll=2)
    for core, early in ((0, early_own), (1, early_other)):
        def rows(k, carry, core=core, early=early):
            part = at((core * 4 + k) * 64, 64)
            kept = early[(y + k) % 4, 0:64, :]
            mid = (kept.astype(f32) + projected[part, :]).astype(bf16)
            middle[part, :] = mid
            wide = mid.astype(f32)
            factor = lax.rsqrt(jnp.mean(wide * wide, axis=1, keepdims=True) + epsilon)
            normed[part, :] = (wide * factor * gain[...].astype(f32)).astype(bf16)
            return carry

        lax.fori_loop(0, 4, rows, 0, unroll=2)


OFFSETS = (0, -1, 1, -2, 2, -3, 3, -4)
X_OFFSETS = (0, -1, 1, 2)


def up_kernel(slots, final, normed, *refs):
    if final:
        units, (before, out, weights) = refs[:2], refs[2:]
    else:
        units, (out, weights) = refs[:len(slots)], refs[len(slots):]
    z, x = lax.axis_index(Z), lax.axis_index(X)
    for j, slot in enumerate(slots):
        chunk = 0 if final else (z + 8 + OFFSETS[slot]) % 8
        for k, offset in enumerate(X_OFFSETS):
            row = at(chunk * 256 + (x + 4 + offset) % 4 * 64, 64)
            unit, start = (units[k // 2], k % 2 * 64) if final else (units[j], k * 64)
            weights[row, :] = unit[start:start + 64, :]
    if final:
        lanes = at((z + 8 + OFFSETS[slots[0]]) % 8 * 256, 256)
    else:
        missing = at((z + 8 + OFFSETS[7]) % 8 * 256, 256)
        weights[missing, :] = jnp.zeros((256, 1024), bf16)

    def columns(n, carry):
        part = at(n * 256, 256)
        if final:
            term = before[:, part] + jnp.dot(normed[:, lanes], weights[:, part], preferred_element_type=f32)
            positive = jnp.maximum(term, 0.0)
            out[:, part] = (positive * positive).astype(bf16)
        else:
            out[:, part] = jnp.dot(normed[...], weights[:, part], preferred_element_type=f32)
        return carry

    lax.fori_loop(0, 4, columns, 0)


def gather_kernel(rows, *refs):
    pieces, out, sems = refs[:-2], refs[-2], refs[-1]
    copy_all([(p, out.at[k * rows:(k + 1) * rows]) for k, p in enumerate(pieces)], sems)


def down_kernel(other_half, hidden, mine, before, after, far_a, far_b, *refs):
    if other_half:
        partial, outs, weights, ordered = refs[0], refs[1:9], refs[9], refs[10]
        ordered[0:256, :] = hidden[256:512, :]
        ordered[256:512, :] = hidden[0:256, :]
    else:
        out, weights = refs
        ordered = hidden
    c, z, x = lax.axis_index(C), lax.axis_index(Z), lax.axis_index(X)
    lanes = at((1 - c if other_half else c) * 1024, 1024)
    for slot in range(8):
        there = (z + 8 + OFFSETS[slot]) % 8 * 128
        far, row = (far_a, slot * 32) if slot < 4 else (far_b, slot * 32 - 128)
        weights[at(there + (x + 2) % 4 * 32, 32), :] = far[row:row + 32, lanes]
        for source, offset in ((mine, 0), (before, -1), (after, 1)):
            to = at(there + (x + 4 + offset) % 4 * 32, 32)
            weights[to, :] = source[slot * 32:slot * 32 + 32, lanes]

    def columns(n, carry):
        part = at(n * 256, 256)
        terms = lax.dot_general(
            ordered[...], weights[part, :], (((1,), (1,)), ((), ())), preferred_element_type=f32
        )
        if other_half:
            terms = (terms + partial[:, part]).astype(bf16)
            for k in range(8):
                outs[k][:, part] = terms[k * 64:k * 64 + 64]
        else:
            out[:, part] = terms
        return carry

    lax.fori_loop(0, 4, columns, 0)


def last_kernel(middle, *refs):
    terms, (out, stacked) = refs[:8], refs[8:]
    c = lax.axis_index(C)
    for core in range(2):
        lanes = at((c + core) % 2 * 256, 256)
        for k in range(4):
            for b in range(4):
                row = (b * 4 + k) * 64
                stacked[row:row + 64, lanes] = terms[core * 4 + k][:, b * 256:b * 256 + 256]
    s = lax.broadcasted_iota(jnp.int32, (512, 512), 0)
    d = lax.broadcasted_iota(jnp.int32, (512, 512), 1)
    wanted = ((s % 256) // 32) * 64 + (s // 256) * 32 + s % 32
    turn = (wanted == d).astype(f32).astype(bf16)
    for b in range(4):
        spread = jnp.dot(stacked[b * 256:b * 256 + 256, :], turn, preferred_element_type=f32)
        summed = spread[0:64] + spread[64:128] + spread[128:192] + spread[192:256]
        part = slice(b * 512, b * 512 + 512)
        out[:, part] = (middle[0:64, part].astype(f32) + summed).astype(bf16)


def shift(value, axis, by):
    n = lax.axis_size(axis)
    return lax.ppermute(value, axis, [(i, (i + by) % n) for i in range(n)])


def to_peer(value, core, by):
    pairs = [(c * 4 + y, (c ^ core) * 4 + (y + by) % 4) for c in range(2) for y in range(4)]
    return lax.ppermute(value, (C, Y), pairs)


def z_ring(piece, steps=4):
    up, down = [piece], [piece]
    for step in range(steps):
        up.append(shift(up[-1], Z, 1))
        if step < 3:
            down.append(shift(down[-1], Z, -1))
    return [piece, up[1], down[1], up[2], down[2], up[3], down[3], *up[4:]]


def half_kernel(one, two, first, second, sems):
    rows = first.shape[0]
    copy_all([(one.at[0:rows], first), (two.at[rows:2 * rows], second)], sems)


def half_of_each(one, two):
    half = jax.ShapeDtypeStruct((one.shape[0] // 2, one.shape[1]), one.dtype)
    return call(
        half_kernel,
        [half, half],
        [ANY] * 2,
        (one, two),
        scratch=[pltpu.SemaphoreType.DMA((2,))],
        flops=1_000_000,
        vmem=4,
    )


def layer(
    residual,
    query_vectors,
    key_vectors,
    value_vectors,
    in_gate,
    forget_gate,
    documents,
    w_out,
    norm_gain,
    w_up,
    w_down,
):
    c = lax.axis_index(C)
    first = c == 0
    left, right = w_up[:, :1024], w_up[:, 1024:]
    keep, give = jnp.where(first, left, right), jnp.where(first, right, left)
    taken = shift(give, C, 1)
    mine = jnp.where(
        first, jnp.concatenate([keep, taken], axis=0), jnp.concatenate([taken, keep], axis=0)
    )
    across = [mine, shift(mine, X, 1), shift(mine, X, -1), shift(mine, X, 2)]
    unit = call(
        functools.partial(gather_kernel, 64),
        jax.ShapeDtypeStruct((256, 1024), bf16),
        [ANY] * 4,
        across,
        scratch=[pltpu.SemaphoreType.DMA((4,))],
        flops=1_000_000,
        vmem=4,
    )
    up_units = z_ring(unit, 3)
    far_up, far_down = half_of_each(up_units[5], up_units[6])
    far_up, far_down = shift(far_up, Z, 1), shift(far_down, Z, -1)
    down_columns = call(
        functools.partial(gather_kernel, 32),
        jax.ShapeDtypeStruct((256, 2048), bf16),
        [ANY] * 8,
        z_ring(w_down.T),
        scratch=[pltpu.SemaphoreType.DMA((8,))],
        flops=1_000_000,
        vmem=4,
    )
    before, after = shift(down_columns, X, 1), shift(down_columns, X, -1)
    far_a, far_b = half_of_each(before, after)
    far_a, far_b = shift(far_a, X, 1), shift(far_b, X, -1)
    docs = documents.reshape(1, -1)
    tokens = query_vectors.shape[0]
    pair = pltpu.VMEM((tokens, 128), bf16)
    state, packed = call(
        memory_kernel,
        [
            jax.ShapeDtypeStruct((STATE_ROWS, 128), f32),
            jax.ShapeDtypeStruct((tokens, 768), f32),
        ],
        [HBM] * 6,
        (in_gate, forget_gate, docs, query_vectors, key_vectors, value_vectors),
        scratch=[
            pltpu.VMEM(in_gate.shape, f32),
            pltpu.VMEM(in_gate.shape, f32),
            pltpu.VMEM(docs.shape, jnp.int32),
            pair,
            pair,
            pair,
            pltpu.SemaphoreType.DMA((6,)),
        ],
        flops=150_000_000,
    )
    received = [
        lax.ppermute(state, (Z, X), [(i, (i + back) % 32) for i in range(32)])
        for back in range(1, CHIPS_BACK + 1)
    ]
    states = call(
        functools.partial(gather_kernel, STATE_ROWS),
        jax.ShapeDtypeStruct((STATE_ROWS * (CHIPS_BACK + 1), 128), f32),
        [ANY] * (CHIPS_BACK + 1),
        (state, *received),
        scratch=[pltpu.SemaphoreType.DMA((CHIPS_BACK + 1,))],
        flops=1_000_000,
        vmem=4,
    )
    other = shift(states, C, 1)
    early = call(
        early_kernel,
        jax.ShapeDtypeStruct((4, 128, 2048), bf16),
        [HBM] * 2,
        (residual, w_out),
        scratch=[pltpu.SemaphoreType.DMA((8,))],
        flops=1_000_000,
        vmem=4,
    )
    early_own = lax.all_to_all(early, Y, 0, 0, tiled=True)
    early_other = shift(early_own, C, 1)
    mixed = call(
        merge_kernel,
        jax.ShapeDtypeStruct((tokens, 128), bf16),
        [VM] * 3,
        (packed, states, other),
        flops=100_000_000,
    )
    peers = [(core, by) for core in range(2) for by in range(4)]
    mixes = call(
        functools.partial(gather_kernel, tokens),
        jax.ShapeDtypeStruct((4 * tokens, 128), bf16),
        [ANY] * 4,
        [mixed] + [to_peer(mixed, 0, back) for back in range(1, 4)],
        scratch=[pltpu.SemaphoreType.DMA((4,))],
        flops=1_000_000,
        vmem=4,
    )
    mixes_other = shift(mixes, C, 1)
    rows_here = jax.ShapeDtypeStruct((512, 2048), bf16)
    middle, normed = call(
        middle_kernel,
        [rows_here] * 2,
        [VM] * 5,
        (early_own, early_other, norm_gain.reshape(1, -1), mixes, mixes_other),
        scratch=[
            pltpu.VMEM((512, 2048), bf16),
            pltpu.VMEM((512, 512), bf16),
            pltpu.VMEM((512, 2048), f32),
        ],
        flops=2 * 512 * 512 * 2048,
    )
    early_slots = tuple(range(7))
    summed = call(
        functools.partial(up_kernel, early_slots, False),
        jax.ShapeDtypeStruct((512, 1024), f32),
        [VM] * 8,
        (normed, *up_units[:7]),
        scratch=[pltpu.VMEM((2048, 1024), bf16)],
        flops=2 * 512 * 1024 * 1792,
    )
    hidden = call(
        functools.partial(up_kernel, (7,), True),
        jax.ShapeDtypeStruct((512, 1024), bf16),
        [VM] * 4,
        (normed, far_up, far_down, summed),
        scratch=[pltpu.VMEM((256, 1024), bf16)],
        flops=2 * 512 * 1024 * 256,
    )
    hidden_other = shift(hidden, C, 1)
    pieces = (down_columns, before, after, far_a, far_b)
    space = pltpu.VMEM((1024, 1024), bf16)
    partial = call(
        functools.partial(down_kernel, False),
        jax.ShapeDtypeStruct((512, 1024), f32),
        [VM] * 6,
        (hidden, *pieces),
        scratch=[space],
        flops=512 * 1024 * 2048,
    )
    sent = call(
        functools.partial(down_kernel, True),
        [jax.ShapeDtypeStruct((64, 1024), bf16)] * 8,
        [VM] * 7,
        (hidden_other, *pieces, partial),
        scratch=[space, pltpu.VMEM((512, 1024), bf16)],
        flops=512 * 1024 * 2048,
    )
    terms = [sent[0]] + [to_peer(sent[k], *peer) for k, peer in enumerate(peers) if k]
    return call(
        last_kernel,
        jax.ShapeDtypeStruct((64, 2048), bf16),
        [VM] * 9,
        (middle, *terms),
        scratch=[pltpu.VMEM((1024, 512), bf16)],
        flops=2 * 1024 * 512 * 512,
    )


def solution(mesh):
    torus = Mesh(mesh.devices.reshape(8, 4, 2, mesh.shape["tp"]), SP_TP)
    in_specs = (
        P(SP_TP, None),
        P(SP, "tp"),
        P(SP, "tp"),
        P(SP, "tp"),
        P("tp", SP),
        P("tp", SP),
        P(SP),
        P("tp", None),
        P(),
        P(SP, "tp"),
        P("tp", SP),
    )
    out_specs = P(SP_TP, None)
    return jax.shard_map(layer, mesh=torus, in_specs=in_specs, out_specs=out_specs, check_vma=False)
```

```python
import functools

import jax
import jax.numpy as jnp
from jax import lax
from jax.experimental import pallas as pl
from jax.experimental.pallas import tpu as pltpu
from jax.sharding import Mesh
from jax.sharding import PartitionSpec as P


SP = ("sp_0", "sp_1", "sp_2")
SP_TP = ("sp_0", "sp_1", "sp_2", "tp")
Z, X, C, Y = SP_TP
CHIPS_BACK = 4
very_negative = -1e30
epsilon = 1e-06
f32 = jnp.float32
bf16 = jnp.bfloat16
HIGH = lax.Precision.HIGHEST

VM = pl.BlockSpec(memory_space=pltpu.VMEM)
SM = pl.BlockSpec(memory_space=pltpu.SMEM)
ANY = pl.BlockSpec(memory_space=pl.ANY)
HBM = pl.BlockSpec(memory_space=pltpu.HBM)


def call(kernel, outs, ins, args, scratch=(), flops=1, traffic=1, vmem=16):
    many = isinstance(outs, (list, tuple))
    return pl.pallas_call(
        kernel,
        out_shape=outs,
        in_specs=ins,
        out_specs=[VM] * len(outs) if many else VM,
        scratch_shapes=list(scratch),
        cost_estimate=pl.CostEstimate(flops=flops, bytes_accessed=traffic, transcendentals=0),
        compiler_params=pltpu.CompilerParams(vmem_limit_bytes=vmem * 1024 * 1024),
    )(*args)


def halves(shape, zero, one):
    lane = lax.broadcasted_iota(jnp.int32, shape, 1)
    return jnp.where(lane < 64, zero, one)


def copy_all(pairs, sems):
    copies = [pltpu.make_async_copy(a, b, sems.at[k]) for k, (a, b) in enumerate(pairs)]
    for c in copies:
        c.start()
    for c in copies:
        c.wait()


def at(start, size):
    return pl.ds(pl.multiple_of(start, size), size)


STATE_ROWS = 72


def memory_kernel(*refs):
    state, packed = refs[6:8]
    in_gate, forget_gate, docs, queries, keys, values = refs[8:14]
    copy_all(list(zip(refs[:6], refs[8:14])), refs[14])
    forget = forget_gate[...]
    decay = jnp.minimum(forget, 0.0) - jnp.log1p(jnp.exp(-jnp.abs(forget)))
    lane = lax.broadcasted_iota(jnp.int32, decay.shape, 1)
    total = decay
    step = 1
    while step < decay.shape[1]:
        total = total + jnp.where(lane >= step, pltpu.roll(total, step, 1), 0.0)
        step *= 2
    gate = in_gate[...]
    doc = docs[...].astype(f32)
    table = jnp.concatenate([total, gate, doc, jnp.zeros((3, doc.shape[1]), f32)], axis=0)
    turned = jnp.transpose(table)
    last = doc[:, -1:]
    end = total[:, -1:]
    growth = jnp.where(doc == last, end - total + gate, very_negative)
    top = jnp.max(growth, axis=1, keepdims=True)
    latest = turned[:, 4:5] == last
    weight = []
    for h in range(2):
        grown = jnp.where(latest, end[h:h + 1] - turned[:, h:h + 1] + turned[:, 2 + h:3 + h], very_negative)
        weight.append(jnp.exp(grown - top[h:h + 1]))
    wide = halves(keys.shape, weight[0], weight[1])
    weighted = wide * keys[...].astype(f32)
    full = jnp.dot(jnp.transpose(weighted), values[...].astype(f32), precision=HIGH, preferred_element_type=f32)
    state[0:64, :] = halves((64, 128), full[0:64], full[64:128])
    normal = jnp.sum(weighted, axis=0, keepdims=True)
    tail = [
        normal,
        halves((1, 128), top[0:1], top[1:2]),
        halves((1, 128), end[0:1], end[1:2]),
        jnp.broadcast_to(last, (1, 128)),
        jnp.zeros((4, 128), f32),
    ]
    state[64:72, :] = jnp.concatenate(tail, axis=0)

    length = queries.shape[0]
    scaled = queries[...] * jnp.asarray(0.125, bf16)
    key = keys[...]
    value = values[...]
    row_ids = lax.broadcasted_iota(jnp.int32, (length, length), 0)
    col_ids = lax.broadcasted_iota(jnp.int32, (length, length), 1)
    allowed = (col_ids <= row_ids) & (turned[:, 4:5] == doc)
    found = []
    for h in range(2):
        inside = jnp.where(
            allowed,
            turned[:, h:h + 1] - total[h:h + 1, :] + gate[h:h + 1, :],
            very_negative,
        )
        peak = jnp.max(inside, axis=1, keepdims=True)
        mine = halves(key.shape, jnp.asarray(1 - h, bf16), jnp.asarray(h, bf16)) * key
        scores = lax.dot_general(scaled, mine, (((1,), (1,)), ((), ())), preferred_element_type=f32)
        weight = jnp.exp(inside - peak) * scores
        summed = jnp.dot(weight.astype(bf16), value, preferred_element_type=f32)
        found.append((summed, jnp.sum(weight, axis=1, keepdims=True), peak, turned[:, h:h + 1]))
    for k in range(4):
        packed[:, k * 128:k * 128 + 128] = halves((length, 128), found[0][k], found[1][k])
    packed[:, 512:640] = jnp.broadcast_to(turned[:, 4:5], (length, 128))
    packed[:, 640:768] = scaled.astype(f32)


def merge_kernel(packed, states_own, other, mixed):
    numer, denom, inner, moved, doc, scaled = (packed[:, k * 128:k * 128 + 128] for k in range(6))
    c = lax.axis_index(C)
    chip = lax.axis_index(Z) * 4 + lax.axis_index(X)
    upper = jnp.zeros((1, 128), jnp.int32) + c == 1
    chips = jnp.zeros((1, 128), jnp.int32) + chip
    states = [(other[0:STATE_ROWS], upper)]
    for back in range(1, CHIPS_BACK + 1):
        there = slice(back * STATE_ROWS, (back + 1) * STATE_ROWS)
        mine, theirs = states_own[there], other[there]
        states.append((jnp.where(c == 1, mine, theirs), chips >= back))
        states.append((jnp.where(c == 1, theirs, mine), chips >= back))
    open_doc = jnp.where(upper, states[0][0][67:68], states[1][0][67:68])
    decayed = jnp.zeros((1, 128), f32)
    reach = []
    for state, there in states:
        joined = (state[67:68] == open_doc) & there
        reach.append(jnp.where(joined, state[65:66] + decayed, very_negative))
        decayed = decayed + jnp.where(there, state[66:67], 0.0)
    top = functools.reduce(jnp.maximum, reach)
    memory = jnp.zeros((64, 128), f32)
    normal = jnp.zeros((1, 128), f32)
    for far, (state, _) in zip(reach, states):
        scale = jnp.where(far > 0.5 * very_negative, jnp.exp(far - top), 0.0)
        memory = memory + scale * state[0:64]
        normal = normal + scale * state[64:65]
    open_here = (doc == open_doc) & (top > 0.5 * very_negative)
    outside = jnp.where(open_here, moved + top, very_negative)
    both = jnp.maximum(outside, inner)
    carried = jnp.exp(outside - both)
    kept = jnp.exp(inner - both)
    blocks = jnp.concatenate([halves((64, 128), memory, 0.0), halves((64, 128), 0.0, memory)], axis=0)
    readout = jnp.dot(scaled, blocks, precision=HIGH, preferred_element_type=f32)
    ones = jnp.concatenate([halves((64, 128), 1.0, 0.0), halves((64, 128), 0.0, 1.0)], axis=0)
    along = jnp.dot(scaled * normal, ones, precision=HIGH, preferred_element_type=f32)
    top_part = kept * numer + carried * readout
    low_part = kept * denom + carried * along
    result = (top_part / jnp.maximum(jnp.abs(low_part), jnp.exp(-both))).astype(bf16)
    mixed[...] = result


def early_kernel(residual, w_out, out, sems):
    rows = at(lax.axis_index(C) * 64, 64)
    copy_all(
        [(residual, out.at[k, 0:64]) for k in range(4)]
        + [(w_out.at[rows], out.at[k, 64:128]) for k in range(4)],
        sems,
    )


def middle_kernel(early_own, early_other, gain, mixes_own, mixes_other, middle, normed, weights, heads, projected):
    c, y = lax.axis_index(C), lax.axis_index(Y)
    for core, early in ((0, early_own), (1, early_other)):
        for there in range(4):
            row = at(there * 128 + (c + core) % 2 * 64, 64)
            weights[row, :] = early[there, 64:128, :]
    for core, mixes in ((0, mixes_own), (1, mixes_other)):
        for back in range(4):
            lanes = at((y + 4 - back) % 4 * 128, 128)
            for k in range(4):
                row = (core * 4 + k) * 64
                heads[row:row + 64, lanes] = mixes[at(back * 256 + (y + k) % 4 * 64, 64), :]

    def columns(n, carry):
        part = at(n * 256, 256)
        projected[:, part] = jnp.dot(heads[...], weights[:, part], preferred_element_type=f32)
        return carry

    lax.fori_loop(0, 8, columns, 0, unroll=2)
    for core, early in ((0, early_own), (1, early_other)):
        def rows(k, carry, core=core, early=early):
            part = at((core * 4 + k) * 64, 64)
            kept = early[(y + k) % 4, 0:64, :]
            mid = (kept.astype(f32) + projected[part, :]).astype(bf16)
            middle[part, :] = mid
            wide = mid.astype(f32)
            factor = lax.rsqrt(jnp.mean(wide * wide, axis=1, keepdims=True) + epsilon)
            normed[part, :] = (wide * factor * gain[...].astype(f32)).astype(bf16)
            return carry

        lax.fori_loop(0, 4, rows, 0, unroll=2)


OFFSETS = (0, -1, 1, -2, 2, -3, 3, -4)
X_OFFSETS = (0, -1, 1, 2)


def up_kernel(slots, first, final, normed, *refs):
    count = len(slots) + final
    units, refs = refs[:count], refs[count:]
    before, (out, weights, left) = (None, refs) if first else (refs[0], refs[1:])
    z, x = lax.axis_index(Z), lax.axis_index(X)
    for j, slot in enumerate(slots):
        left[:, j * 256:j * 256 + 256] = normed[:, at((z + 8 + OFFSETS[slot]) % 8 * 256, 256)]
        for k, offset in enumerate(X_OFFSETS):
            row = at(j * 256 + (x + 4 + offset) % 4 * 64, 64)
            unit, start = (units[k // 2], k % 2 * 64) if final else (units[j], k * 64)
            weights[row, :] = unit[start:start + 64, :]

    def columns(n, carry):
        part = at(n * 256, 256)
        term = jnp.dot(left[...], weights[:, part], preferred_element_type=f32)
        if not first:
            term = term + before[:, part]
        if final:
            positive = jnp.maximum(term, 0.0)
            term = (positive * positive).astype(bf16)
        out[:, part] = term
        return carry

    lax.fori_loop(0, 4, columns, 0)


def gather_kernel(rows, *refs):
    pieces, out, sems = refs[:-2], refs[-2], refs[-1]
    copy_all([(p, out.at[k * rows:(k + 1) * rows]) for k, p in enumerate(pieces)], sems)


def down_kernel(other_half, hidden, mine, before, after, far_a, far_b, *refs):
    if other_half:
        partial, outs, weights, ordered = refs[0], refs[1:9], refs[9], refs[10]
        ordered[0:256, :] = hidden[256:512, :]
        ordered[256:512, :] = hidden[0:256, :]
    else:
        out, weights = refs
        ordered = hidden
    c, z, x = lax.axis_index(C), lax.axis_index(Z), lax.axis_index(X)
    lanes = at((1 - c if other_half else c) * 1024, 1024)
    for slot in range(8):
        there = (z + 8 + OFFSETS[slot]) % 8 * 128
        far, row = (far_a, slot * 32) if slot < 4 else (far_b, slot * 32 - 128)
        weights[at(there + (x + 2) % 4 * 32, 32), :] = far[row:row + 32, lanes]
        for source, offset in ((mine, 0), (before, -1), (after, 1)):
            to = at(there + (x + 4 + offset) % 4 * 32, 32)
            weights[to, :] = source[slot * 32:slot * 32 + 32, lanes]

    def columns(n, carry):
        part = at(n * 256, 256)
        terms = lax.dot_general(
            ordered[...], weights[part, :], (((1,), (1,)), ((), ())), preferred_element_type=f32
        )
        if other_half:
            terms = (terms + partial[:, part]).astype(bf16)
            for k in range(8):
                outs[k][:, part] = terms[k * 64:k * 64 + 64]
        else:
            out[:, part] = terms
        return carry

    lax.fori_loop(0, 4, columns, 0)


def last_kernel(middle, *refs):
    terms, (out, stacked) = refs[:8], refs[8:]
    c = lax.axis_index(C)
    for core in range(2):
        lanes = at((c + core) % 2 * 256, 256)
        for k in range(4):
            for b in range(4):
                row = (b * 4 + k) * 64
                stacked[row:row + 64, lanes] = terms[core * 4 + k][:, b * 256:b * 256 + 256]
    s = lax.broadcasted_iota(jnp.int32, (512, 512), 0)
    d = lax.broadcasted_iota(jnp.int32, (512, 512), 1)
    wanted = ((s % 256) // 32) * 64 + (s // 256) * 32 + s % 32
    turn = (wanted == d).astype(f32).astype(bf16)
    for b in range(4):
        spread = jnp.dot(stacked[b * 256:b * 256 + 256, :], turn, preferred_element_type=f32)
        summed = spread[0:64] + spread[64:128] + spread[128:192] + spread[192:256]
        part = slice(b * 512, b * 512 + 512)
        out[:, part] = (middle[0:64, part].astype(f32) + summed).astype(bf16)


def shift(value, axis, by):
    n = lax.axis_size(axis)
    return lax.ppermute(value, axis, [(i, (i + by) % n) for i in range(n)])


def to_peer(value, core, by):
    pairs = [(c * 4 + y, (c ^ core) * 4 + (y + by) % 4) for c in range(2) for y in range(4)]
    return lax.ppermute(value, (C, Y), pairs)


def z_ring(piece, steps=4):
    up, down = [piece], [piece]
    for step in range(steps):
        up.append(shift(up[-1], Z, 1))
        if step < 3:
            down.append(shift(down[-1], Z, -1))
    return [piece, up[1], down[1], up[2], down[2], up[3], down[3], *up[4:]]


def half_kernel(one, two, first, second, sems):
    rows = first.shape[0]
    copy_all([(one.at[0:rows], first), (two.at[rows:2 * rows], second)], sems)


def half_of_each(one, two):
    half = jax.ShapeDtypeStruct((one.shape[0] // 2, one.shape[1]), one.dtype)
    return call(
        half_kernel,
        [half, half],
        [ANY] * 2,
        (one, two),
        scratch=[pltpu.SemaphoreType.DMA((2,))],
        flops=1_000_000,
        vmem=4,
    )


def layer(
    residual,
    query_vectors,
    key_vectors,
    value_vectors,
    in_gate,
    forget_gate,
    documents,
    w_out,
    norm_gain,
    w_up,
    w_down,
):
    c = lax.axis_index(C)
    first = c == 0
    left, right = w_up[:, :1024], w_up[:, 1024:]
    keep, give = jnp.where(first, left, right), jnp.where(first, right, left)
    taken = shift(give, C, 1)
    mine = jnp.where(
        first, jnp.concatenate([keep, taken], axis=0), jnp.concatenate([taken, keep], axis=0)
    )
    across = [mine, shift(mine, X, 1), shift(mine, X, -1), shift(mine, X, 2)]
    unit = call(
        functools.partial(gather_kernel, 64),
        jax.ShapeDtypeStruct((256, 1024), bf16),
        [ANY] * 4,
        across,
        scratch=[pltpu.SemaphoreType.DMA((4,))],
        flops=1_000_000,
        vmem=4,
    )
    up_units = z_ring(unit, 3)
    down_columns = call(
        functools.partial(gather_kernel, 32),
        jax.ShapeDtypeStruct((256, 2048), bf16),
        [ANY] * 8,
        z_ring(w_down.T),
        scratch=[pltpu.SemaphoreType.DMA((8,))],
        flops=1_000_000,
        vmem=4,
    )
    before, after = shift(down_columns, X, 1), shift(down_columns, X, -1)
    docs = documents.reshape(1, -1)
    tokens = query_vectors.shape[0]
    pair = pltpu.VMEM((tokens, 128), bf16)
    state, packed = call(
        memory_kernel,
        [
            jax.ShapeDtypeStruct((STATE_ROWS, 128), f32),
            jax.ShapeDtypeStruct((tokens, 768), f32),
        ],
        [HBM] * 6,
        (in_gate, forget_gate, docs, query_vectors, key_vectors, value_vectors),
        scratch=[
            pltpu.VMEM(in_gate.shape, f32),
            pltpu.VMEM(in_gate.shape, f32),
            pltpu.VMEM(docs.shape, jnp.int32),
            pair,
            pair,
            pair,
            pltpu.SemaphoreType.DMA((6,)),
        ],
        flops=150_000_000,
    )
    received = [
        lax.ppermute(state, (Z, X), [(i, (i + back) % 32) for i in range(32)])
        for back in range(1, CHIPS_BACK + 1)
    ]
    states = call(
        functools.partial(gather_kernel, STATE_ROWS),
        jax.ShapeDtypeStruct((STATE_ROWS * (CHIPS_BACK + 1), 128), f32),
        [ANY] * (CHIPS_BACK + 1),
        lax.optimization_barrier((state, *received, down_columns))[:-1],
        scratch=[pltpu.SemaphoreType.DMA((CHIPS_BACK + 1,))],
        flops=1_000_000,
        vmem=4,
    )
    other = shift(states, C, 1)
    early = call(
        early_kernel,
        jax.ShapeDtypeStruct((4, 128, 2048), bf16),
        [HBM] * 2,
        lax.optimization_barrier((residual, w_out, unit))[:2],
        scratch=[pltpu.SemaphoreType.DMA((8,))],
        flops=1_000_000,
        vmem=4,
    )
    early_own = lax.all_to_all(early, Y, 0, 0, tiled=True)
    early_other = shift(early_own, C, 1)
    mixed = call(
        merge_kernel,
        jax.ShapeDtypeStruct((tokens, 128), bf16),
        [VM] * 3,
        (packed, states, other),
        flops=100_000_000,
    )
    peers = [(core, by) for core in range(2) for by in range(4)]
    mixes = call(
        functools.partial(gather_kernel, tokens),
        jax.ShapeDtypeStruct((4 * tokens, 128), bf16),
        [ANY] * 4,
        [mixed] + [to_peer(mixed, 0, back) for back in range(1, 4)],
        scratch=[pltpu.SemaphoreType.DMA((4,))],
        flops=1_000_000,
        vmem=4,
    )
    mixes_other = shift(mixes, C, 1)
    rows_here = jax.ShapeDtypeStruct((512, 2048), bf16)
    middle, normed = call(
        middle_kernel,
        [rows_here] * 2,
        [VM] * 5,
        (early_own, early_other, norm_gain.reshape(1, -1), mixes, mixes_other),
        scratch=[
            pltpu.VMEM((512, 2048), bf16),
            pltpu.VMEM((512, 512), bf16),
            pltpu.VMEM((512, 2048), f32),
        ],
        flops=2 * 512 * 512 * 2048,
    )
    ready = lax.optimization_barrier((before, after, normed))
    far_a, far_b = half_of_each(ready[0], ready[1])
    far_a, far_b, normed = lax.optimization_barrier((far_a, far_b, normed))
    far_a, far_b = shift(far_a, X, 1), shift(far_b, X, -1)

    def up(slots, units, summed, final=False):
        return call(
            functools.partial(up_kernel, slots, not summed, final),
            jax.ShapeDtypeStruct((512, 1024), bf16 if final else f32),
            [VM] * (1 + len(units) + len(summed)),
            (normed, *units, *summed),
            scratch=[
                pltpu.VMEM((256 * len(slots), 1024), bf16),
                pltpu.VMEM((512, 256 * len(slots)), bf16),
            ],
            flops=2 * 512 * 1024 * 256 * len(slots),
        )

    summed = up((0, 1, 2, 3, 4), up_units[:5], ())
    ready = lax.optimization_barrier((up_units[5], up_units[6], normed))
    far_up, far_down = half_of_each(ready[0], ready[1])
    far_up, far_down = shift(far_up, Z, 1), shift(far_down, Z, -1)
    summed = up((5, 6), up_units[5:7], (summed,))
    hidden = up((7,), (far_up, far_down), (summed,), True)
    hidden_other = shift(hidden, C, 1)
    pieces = (down_columns, before, after, far_a, far_b)
    space = pltpu.VMEM((1024, 1024), bf16)
    partial = call(
        functools.partial(down_kernel, False),
        jax.ShapeDtypeStruct((512, 1024), f32),
        [VM] * 6,
        (hidden, *pieces),
        scratch=[space],
        flops=512 * 1024 * 2048,
    )
    sent = call(
        functools.partial(down_kernel, True),
        [jax.ShapeDtypeStruct((64, 1024), bf16)] * 8,
        [VM] * 7,
        (hidden_other, *pieces, partial),
        scratch=[space, pltpu.VMEM((512, 1024), bf16)],
        flops=512 * 1024 * 2048,
    )
    terms = [sent[0]] + [to_peer(sent[k], *peer) for k, peer in enumerate(peers) if k]
    return call(
        last_kernel,
        jax.ShapeDtypeStruct((64, 2048), bf16),
        [VM] * 9,
        (middle, *terms),
        scratch=[pltpu.VMEM((1024, 512), bf16)],
        flops=2 * 1024 * 512 * 512,
    )


def solution(mesh):
    torus = Mesh(mesh.devices.reshape(8, 4, 2, mesh.shape["tp"]), SP_TP)
    in_specs = (
        P(SP_TP, None),
        P(SP, "tp"),
        P(SP, "tp"),
        P(SP, "tp"),
        P("tp", SP),
        P("tp", SP),
        P(SP),
        P("tp", None),
        P(),
        P(SP, "tp"),
        P("tp", SP),
    )
    out_specs = P(SP_TP, None)
    return jax.shard_map(layer, mesh=torus, in_specs=in_specs, out_specs=out_specs, check_vma=False)
```
